32 devices in a mesh: ep: 8 (over z, x), tp: 4 (over y, core).
Axes of the slice: x: 2, y: 2, z: 4, core: 2. Of those that a mesh axis runs over, the one named last changes fastest.
Arguments:
- tokens: bfloat16 [5120, 2048], P(('ep', 'tp')), may hold values from -6 to 6
- expert_ids: int32 [5120, 2], P(('ep', 'tp')), may hold values from 0 to 7, all different within a row; in each aligned block of 160 rows (0 to 159, 160 to 319, ...) at most 60 rows name the same one
- group_weight: float32 [5120], P(('ep', 'tp')), may hold values from 0.3 to 1
- expert_share: float32 [5120, 2], P(('ep', 'tp')), may hold values from 0.05 to 1
- gate_w: bfloat16 [8, 512, 2048], P('ep', 'tp'), may hold values from -0.125 to 0.125
- up_w: bfloat16 [8, 512, 2048], P('ep', 'tp'), may hold values from -0.125 to 0.125
- down_w: bfloat16 [8, 512, 2048], P('ep', 'tp'), may hold values from -0.25 to 0.25
- out_gain: float32 [2048], replicated, may hold values from 0.1 to 1.9
- out_shift: float32 [2048], replicated, may hold values from -3 to 3
Outputs:
- layer_out: bfloat16 [5120, 2048], P(('ep', 'tp'))
The draws below stay inside these ranges and needn't reach their ends.
Inputs may be any that keep to these rules, and one draw needn't show every extreme that they name: `expert_ids`: the 2 ids of a token differ. Among the rows of one device no id is named more than 60 times, and in some device's rows some id is named exactly 60 times.
All inputs are finite; a program needn't handle non-finite values.
Results may differ from the reference program's by a relative error of at most 0.0021.
Values may be sent and summed in bfloat16 or wider, within the bound.
A program may use at most 64 MiB of HBM per device.

```python
import math
import jax
import jax.numpy as jnp
import numpy as np
from jax import lax

D = 2048
FF = 512
TOP = 2
TOK_DEV = 160
EXPERTS = 8
CAP = 60
TOKENS = 5120
N_EP = 8
N_TP = 4


def block_scale(key, extent, cuts, least, top_value):
    def one(dim, blocks):
        draws = jax.random.uniform(jax.random.fold_in(jax.random.fold_in(key, 6), dim), (blocks,), jnp.float32, least / len(cuts), top_value / len(cuts))
        return jnp.repeat(jnp.exp(draws), extent[dim] // blocks).reshape((-1,) + (1,) * (len(extent) - dim - 1))

    loudness = one(*cuts[0])
    for cut in cuts[1:]:
        loudness = loudness * one(*cut)
    return loudness


def assign_block(key, own, number, rows, amount, top, reach, skew):
    sequence = jax.random.permutation(key, amount)
    crowded, common = shares(amount, rows * top, reach, skew, True), shares(amount, rows * top, reach, skew, False)
    places = jnp.arange(amount)

    def named(sizes, offset_by):
        used = int((sizes > 0).sum())
        fixed = max(1, used // 4)
        shifted = fixed + (places - fixed + offset_by * (used - fixed)) % max(1, amount - fixed)
        return jnp.zeros((amount,), jnp.int32).at[sequence[jnp.where(places < fixed, places, shifted)]].set(jnp.asarray(sizes, jnp.int32))

    sizes = jnp.where(number % 4 == 0, named(crowded, number // 4), named(common, number - number // 4 - 1))
    mixed = jax.random.permutation(jax.random.fold_in(own, 3), amount)
    source_of, receiver = mixed[0:amount // 2 * 2:2], mixed[1:amount // 2 * 2:2]
    slack = jnp.minimum(sizes[source_of] - 1, reach - sizes[receiver]) // 2
    slack = jnp.where((source_of == sequence[0]) | (receiver == sequence[0]) | (sizes[receiver] == 0), 0, jnp.maximum(slack, 0))
    shifted = jax.random.randint(jax.random.fold_in(own, 4), (amount // 2,), 0, 1 << 20) % (slack + 1)
    sizes = sizes.at[source_of].add(-shifted).at[receiver].add(shifted)
    items = jnp.searchsorted(jnp.cumsum(sizes), jnp.arange(rows * top), side="right").astype(jnp.int32)
    table = items.reshape(top, rows).T
    table = table[jax.random.permutation(jax.random.fold_in(own, 1), rows)]
    offset_by = jax.random.randint(jax.random.fold_in(own, 2), (rows, 1), 0, top)
    return jnp.take_along_axis(table, (jnp.arange(top)[None, :] + offset_by) % top, axis=1)


def shares(amount, total, reach, lean, full):
    weights = [(1 << 20) // math.isqrt(rank ** lean) + 1 for rank in range(1, amount + 1)]
    largest = reach if full else min(reach, max(-(-total // amount), total * weights[0] // sum(weights)))
    least = 1 if total - largest >= amount - 1 else 0
    given, rest = [largest] + [least] * (amount - 1), total - largest - least * (amount - 1)
    while rest > 0:
        movable = [i for i in range(1, amount) if given[i] < largest] or [i for i in range(1, amount) if given[i] < reach]
        pool, budget = sum([weights[i] for i in movable]), rest
        for i in movable:
            more = min(reach - given[i], max(1, budget * weights[i] // pool), rest)
            given[i] = given[i] + more
            rest = rest - more
    return np.array(given)


def centred(stream_key, shape, spread, limit, pieces=(), held_as=jnp.bfloat16):
    result = jax.random.normal(stream_key, shape, jnp.float32) * spread
    if len(pieces) > 0:
        result = block_scale(stream_key, shape, pieces, -0.22, 0.18) * result
    return jnp.clip(result, min=-limit, max=limit).astype(held_as)


def setup_inputs(seed: int = 0) -> dict:
    streams_of = jax.random.split(jax.random.key(seed), 10)
    tokens = centred(streams_of[0], (TOKENS, D), 1.0, 6.0, ((0, 32),))
    expert_ids_keys = jax.random.split(jax.random.fold_in(streams_of[1], 1), TOKENS // TOK_DEV)
    expert_ids_turns = jax.random.permutation(jax.random.fold_in(streams_of[1], 3), TOKENS // TOK_DEV)
    expert_ids = jax.vmap(lambda own, number: assign_block(jax.random.fold_in(streams_of[1], 2), own, number, TOK_DEV, EXPERTS, TOP, CAP, 2))(expert_ids_keys, expert_ids_turns).reshape((TOKENS, TOP))
    group_weight = jnp.clip(0.3 + 0.7 * jax.random.uniform(streams_of[2], (TOKENS,), jnp.float32) ** block_scale(streams_of[2], (TOKENS,), ((0, 32),), -0.2, 0.2), 0.3, 1.0)
    expert_share = jnp.clip(jnp.exp(math.log(1.0) - 2.9957323 * jax.random.uniform(streams_of[3], (TOKENS, TOP), jnp.float32) ** block_scale(streams_of[3], (TOKENS, TOP), ((0, 32),), -0.2, 0.2)), 0.05, 1.0)
    gate_w = centred(streams_of[4], (EXPERTS, FF, D), D ** -0.5, 0.125, ((0, 8), (1, 4)))
    up_w = centred(streams_of[5], (EXPERTS, FF, D), D ** -0.5, 0.125, ((0, 8), (1, 4)))
    down_w = centred(streams_of[6], (EXPERTS, FF, D), FF ** -0.5, 0.25, ((0, 8), (1, 4)))
    out_gain = jnp.clip(1.0 + 0.18 * jax.random.normal(streams_of[7], (D,), jnp.float32), 0.1, 1.9)
    out_shift = centred(streams_of[8], (D,), 0.5, 3.0, (), jnp.float32)
    return {"tokens": tokens, "expert_ids": expert_ids, "group_weight": group_weight, "expert_share": expert_share, "gate_w": gate_w, "up_w": up_w, "down_w": down_w, "out_gain": out_gain, "out_shift": out_shift}


residual_scale = 2.0 ** 0.5
norm_eps = 1e-05

def layer_norm(values, gain, shift):
    center = values - lax.optimization_barrier(jnp.mean(values, axis=-1, keepdims=True))
    variance = lax.optimization_barrier(jnp.mean(center * center, axis=-1, keepdims=True))
    return (center * lax.rsqrt(variance + norm_eps) * gain + shift).astype(jnp.bfloat16)

def reference(tokens, expert_ids, group_weight, expert_share, gate_w, up_w, down_w, out_gain, out_shift):
    tok_count = tokens.shape[0]
    model_width = tokens.shape[1]
    row_limit = N_EP * N_TP * CAP
    share_norm = expert_share / lax.optimization_barrier(jnp.sum(expert_share, axis=1, keepdims=True))
    route_weight = group_weight[:, None] * share_norm
    padded = jnp.concatenate([tokens, jnp.zeros((1, model_width), tokens.dtype)], axis=0)

    def one_expert(carry, expert_num):
        is_hit = expert_ids == expert_num
        weight_col = lax.optimization_barrier(jnp.sum(jnp.where(is_hit, route_weight, 0.0), axis=1))
        token_mask = jnp.any(is_hit, axis=1)
        row_index = jnp.nonzero(token_mask, size=row_limit, fill_value=tok_count)[0].astype(jnp.int32)
        row_data = padded[row_index]
        gate_act = jnp.dot(row_data, gate_w[expert_num].T, preferred_element_type=jnp.float32)
        up_act = jnp.dot(row_data, up_w[expert_num].T, preferred_element_type=jnp.float32)
        hidden = (jax.nn.silu(gate_act) * up_act).astype(jnp.bfloat16)
        expert_out = jnp.dot(hidden, down_w[expert_num], preferred_element_type=jnp.float32).astype(jnp.bfloat16)
        padded_weight = jnp.concatenate([weight_col, jnp.zeros((1,), weight_col.dtype)])[row_index]
        carry = carry.at[row_index].add(padded_weight[:, None] * expert_out.astype(jnp.float32))
        return (carry, None)
    start_total = jnp.zeros((tok_count + 1, model_width), jnp.float32)
    mixture, _ = lax.scan(one_expert, start_total, jnp.arange(EXPERTS, dtype=jnp.int32))
    residual = residual_scale * tokens.astype(jnp.float32) + mixture[:tok_count]
    return layer_norm(residual, out_gain, out_shift)
```

```python
import functools

import jax
import jax.numpy as jnp
from jax import lax
from jax.experimental import pallas as pl
from jax.experimental.pallas import tpu as pltpu
from jax.sharding import PartitionSpec as P

TOP = 2


residual_scale = 2.0**0.5
norm_eps = 1e-05


def layer_norm(values, gain, shift):
    center = values - jnp.mean(values, axis=-1, keepdims=True)
    variance = jnp.mean(center * center, axis=-1, keepdims=True)
    return (center * lax.rsqrt(variance + norm_eps) * gain + shift).astype(jnp.bfloat16)


def body(tokens, expert_ids, group_weight, expert_share, gate_w, up_w, down_w, out_gain, out_shift):
    tok_count, model_width = tokens.shape
    ep_size = lax.axis_size("ep")
    local_count = gate_w.shape[0]
    experts_all = ep_size * local_count
    capacity = 3 * tok_count * TOP // (2 * experts_all)
    flat_ids = expert_ids.reshape(-1)
    onehot = (flat_ids[:, None] == jnp.arange(experts_all, dtype=jnp.int32)[None, :]).astype(
        jnp.int32
    )
    earlier = jnp.cumsum(onehot, axis=0) - onehot
    slot_index = jnp.sum(earlier * onehot, axis=1)
    dest_index = flat_ids * capacity + slot_index
    copies = jnp.repeat(tokens, TOP, axis=0)
    send_buf = (
        jnp.zeros((experts_all * capacity, model_width), tokens.dtype).at[dest_index].set(copies)
    )
    send_buf = send_buf.reshape(ep_size, local_count * capacity, model_width)
    received = lax.all_to_all(send_buf, "ep", split_axis=0, concat_axis=0, tiled=True)
    expert_rows = received.reshape(ep_size, local_count, capacity, model_width)
    expert_rows = expert_rows.transpose(1, 0, 2, 3).reshape(
        local_count, ep_size * capacity, model_width
    )
    gate_piece = lax.all_gather(gate_w, "tp", axis=1, tiled=True)
    up_piece = lax.all_gather(up_w, "tp", axis=1, tiled=True)
    down_piece = lax.all_gather(down_w, "tp", axis=1, tiled=True)
    gate_act = jnp.einsum(
        "lrd,lfd->lrf", expert_rows, gate_piece, preferred_element_type=jnp.float32
    )
    up_act = jnp.einsum("lrd,lfd->lrf", expert_rows, up_piece, preferred_element_type=jnp.float32)
    hidden = (jax.nn.silu(gate_act) * up_act).astype(jnp.bfloat16)
    expert_out = jnp.einsum("lrf,lfd->lrd", hidden, down_piece, preferred_element_type=jnp.float32)
    results = expert_out.astype(jnp.bfloat16).reshape(local_count, ep_size, capacity, model_width)
    results = results.transpose(1, 0, 2, 3).reshape(ep_size, local_count * capacity, model_width)
    returned = lax.all_to_all(results, "ep", split_axis=0, concat_axis=0, tiled=True)
    returned = returned.reshape(experts_all * capacity, model_width)
    picked = returned[dest_index].reshape(tok_count, TOP, model_width)
    share_norm = expert_share / jnp.sum(expert_share, axis=1, keepdims=True)
    route_weight = group_weight[:, None] * share_norm
    mixture = jnp.sum(route_weight[:, :, None] * picked.astype(jnp.float32), axis=1)
    residual = residual_scale * tokens.astype(jnp.float32) + mixture
    return layer_norm(residual, out_gain, out_shift)


MESH = pl.DeviceIdType.MESH
CHUNKS = 4


def cdot(a, b):
    return jnp.dot(a, b, preferred_element_type=jnp.float32)


def ndot(a, b, precision=None):
    return lax.dot_general(
        a, b, (((1,), (1,)), ((), ())), precision=precision, preferred_element_type=jnp.float32
    )


def fused(
    half, cap, ids_ref, group_ref, share_ref, tok_ref, gate_ref, up_ref, down_ref, gain_ref,
    shift_ref, out_ref, meta, mmeta, mtok, send_own, send_mir, recv_own, recv_mir, wgu, wd,
    hid_own, hid_mir, res_own, res_mir, ret_own, ret_mir, part, mpart, total, send_sem, recv_sem,
):
    rows, width = tok_ref.shape
    fpart = gate_ref.shape[0]
    fc = width // CHUNKS
    ep, tp = lax.axis_index("ep"), lax.axis_index("tp")
    lo = lax.rem(ep, half)
    base = ep - lo
    mirror = {"ep": lax.rem(ep + half, 2 * half)}
    pair = {"tp": tp + 1 - 2 * lax.rem(tp, 2)}
    across = {"tp": lax.rem(tp + 2, 4)}
    ahead = [{"ep": base + lax.rem(lo + r, half)} for r in range(half)]
    behind = [{"ep": base + lax.rem(lo + half - r, half)} for r in range(half)]

    barrier = pltpu.get_barrier_semaphore()
    peers = [mirror, pair, across] + ahead[1:]
    for peer in peers:
        pl.semaphore_signal(barrier, inc=1, device_id=peer, device_id_type=MESH)
    pl.semaphore_wait(barrier, len(peers))

    started = []

    def send(src, dst, peer):
        i = len(started)
        copy = pltpu.make_async_remote_copy(
            src_ref=src, dst_ref=dst, send_sem=send_sem.at[i], recv_sem=recv_sem.at[i],
            device_id=peer, device_id_type=MESH,
        )
        copy.start()
        started.append(copy)
        return copy

    def cols(c):
        return pl.ds(c * fc, fc)

    def block(r):
        return pl.ds(r * cap, cap)

    meta[...] = jnp.zeros_like(meta)
    share = share_ref[...]
    weight = group_ref[...] * (share / jnp.sum(share, axis=0, keepdims=True))
    meta[0:2, 0:rows] = ids_ref[...].astype(jnp.float32)
    meta[2:4, 0:rows] = weight
    tok_in = [send(tok_ref.at[:, cols(0)], mtok.at[:, cols(0)], mirror)]
    gate_rows, up_rows = pl.ds(0, fpart), pl.ds(fpart, fpart)

    def wrows(s):
        return pl.ds(s * fpart, fpart)

    gate2 = send(gate_ref, wgu.at[2, gate_rows], across)
    up2 = send(up_ref, wgu.at[2, up_rows], across)
    down2 = send(down_ref, wd.at[wrows(2)], across)
    gate1 = send(gate_ref, wgu.at[1, gate_rows], pair)
    up1 = send(up_ref, wgu.at[1, up_rows], pair)
    down1 = send(down_ref, wd.at[wrows(1)], pair)
    meta_in = send(meta, mmeta, mirror)
    for c in range(1, CHUNKS):
        tok_in.append(send(tok_ref.at[:, cols(c)], mtok.at[:, cols(c)], mirror))
    wgu[0, 0:fpart] = gate_ref[...]
    wgu[0, fpart : 2 * fpart] = up_ref[...]
    wd[0:fpart] = down_ref[...]

    earlier = lax.broadcasted_iota(jnp.int32, (rows, rows), 0)
    later = lax.broadcasted_iota(jnp.int32, (rows, rows), 1)
    before = (earlier < later).astype(jnp.bfloat16)
    same = (earlier == later).astype(jnp.float32)
    names = (base + lax.rem(lo + lax.broadcasted_iota(jnp.int32, (8, rows), 0), half)).astype(
        jnp.float32
    )

    def routing(table):
        first, second = table[0:1, 0:rows] == names, table[1:2, 0:rows] == names
        hits = jnp.where(first | second, 1.0, 0.0)
        slots = cdot(hits.astype(jnp.bfloat16), before)
        key = jnp.where(hits > 0.5, slots, -1.0)
        value = jnp.where(first, table[2:3, 0:rows], 0.0) + jnp.where(
            second, table[3:4, 0:rows], 0.0
        )
        place = lax.broadcasted_iota(jnp.int32, (cap, rows), 0).astype(jnp.float32)
        pick = jnp.concatenate(
            [jnp.where(place == key[r : r + 1], 1.0, 0.0) for r in range(half)], axis=0
        ).astype(jnp.bfloat16)
        key_col = ndot(same, key, lax.Precision.HIGHEST)
        value_col = ndot(same, value, lax.Precision.HIGHEST)
        lane = lax.broadcasted_iota(jnp.int32, (rows, half * cap), 1)
        merge = jnp.zeros((rows, half * cap), jnp.float32)
        for r in range(half):
            at = (lane - r * cap).astype(jnp.float32) == key_col[:, r : r + 1]
            at = at & (lane >= r * cap)
            merge = jnp.where(at, value_col[:, r : r + 1], merge)
        high = merge.astype(jnp.bfloat16)
        low = (merge - high.astype(jnp.float32)).astype(jnp.bfloat16)
        return pick, high, low

    def pack(pick, source, send_buf, recv_buf, c):
        packed = cdot(pick, source[:, cols(c)]).astype(jnp.bfloat16)
        recv_buf[block(0), cols(c)] = packed[0:cap]
        send_buf[:, cols(c)] = packed
        return [
            send(send_buf.at[block(r), cols(c)], recv_buf.at[block(r), cols(c)], ahead[r])
            for r in range(1, half)
        ]

    pick, high_own, low_own = routing(meta)
    own_in = []
    for c in range(CHUNKS):
        own_in += pack(pick, tok_ref, send_own, recv_own, c)

    def gate_up(s, recv_buf, hid):
        both = ndot(recv_buf[...], wgu[s])
        gate, up = both[:, 0:fpart], both[:, fpart : 2 * fpart]
        hid[:, wrows(s)] = (gate / (1.0 + jnp.exp(-gate)) * up).astype(jnp.bfloat16)

    meta_in.wait_recv()
    pick, high_mir, low_mir = routing(mmeta)
    mir_in = []
    tok_in[0].wait_recv()
    mir_in += pack(pick, mtok, send_mir, recv_mir, 0)
    gate2.wait_recv()
    gate3 = send(wgu.at[2, gate_rows], wgu.at[3, gate_rows], pair)
    tok_in[1].wait_recv()
    mir_in += pack(pick, mtok, send_mir, recv_mir, 1)
    for copy in own_in + [gate1, up1]:
        copy.wait_recv()
    gate_up(0, recv_own, hid_own)
    gate_up(1, recv_own, hid_own)
    tok_in[2].wait_recv()
    mir_in += pack(pick, mtok, send_mir, recv_mir, 2)
    up2.wait_recv()
    up3 = send(wgu.at[2, up_rows], wgu.at[3, up_rows], pair)
    gate_up(2, recv_own, hid_own)
    tok_in[3].wait_recv()
    mir_in += pack(pick, mtok, send_mir, recv_mir, 3)
    gate3.wait_recv()
    up3.wait_recv()
    gate_up(3, recv_own, hid_own)
    down2.wait_recv()
    down3 = send(wd.at[wrows(2)], wd.at[wrows(3)], pair)
    for copy in mir_in:
        copy.wait_recv()
    for s in range(4):
        gate_up(s, recv_mir, hid_mir)
    down1.wait_recv()
    down3.wait_recv()

    def project(hid, res, ret, c):
        result = cdot(hid[...], wd[:, cols(c)]).astype(jnp.bfloat16)
        ret[block(0), cols(c)] = result[0:cap]
        res[:, cols(c)] = result
        return [
            send(res.at[block(r), cols(c)], ret.at[block(r), cols(c)], behind[r])
            for r in range(1, half)
        ]

    def combine(high, low, ret, c):
        return cdot(high, ret[:, cols(c)]) + cdot(low, ret[:, cols(c)])

    back_mir = [project(hid_mir, res_mir, ret_mir, c) for c in range(CHUNKS)]
    part_in = []
    back_own = []
    for c in range(CHUNKS):
        for copy in back_mir[c]:
            copy.wait_recv()
        part[:, cols(c)] = combine(high_mir, low_mir, ret_mir, c).astype(jnp.bfloat16)
        part_in.append(send(part.at[:, cols(c)], mpart.at[:, cols(c)], mirror))
        back_own.append(project(hid_own, res_own, ret_own, c))

    for c in range(CHUNKS):
        for copy in back_own[c]:
            copy.wait_recv()
        total[:, cols(c)] = (
            residual_scale * tok_ref[:, cols(c)].astype(jnp.float32)
            + combine(high_own, low_own, ret_own, c)
        )
    mean = jnp.zeros((rows, 1), jnp.float32)
    for c in range(CHUNKS):
        part_in[c].wait_recv()
        piece = total[:, cols(c)] + mpart[:, cols(c)].astype(jnp.float32)
        total[:, cols(c)] = piece
        mean = mean + jnp.sum(piece, axis=1, keepdims=True)
    mean = mean / width
    center = total[...] - mean
    variance = jnp.sum(center * center, axis=1, keepdims=True) / width
    out_ref[...] = (
        center * lax.rsqrt(variance + norm_eps) * gain_ref[...] + shift_ref[...]
    ).astype(jnp.bfloat16)
    for copy in started:
        copy.wait_send()


def fast_body(
    tokens, expert_ids, group_weight, expert_share, gate_w, up_w, down_w, out_gain, out_shift
):
    rows, width = tokens.shape
    experts = lax.axis_size("ep")
    half = experts // 2
    fpart = gate_w.shape[1]
    hidden = fpart * lax.axis_size("tp")
    cap = -(-(3 * rows * TOP // (2 * experts)) // 16) * 16
    lanes = -(-rows // 128) * 128
    packed = half * cap
    copies = 10 + CHUNKS * (2 + 4 * (half - 1))
    bf = jnp.bfloat16
    vmem = pl.BlockSpec(memory_space=pltpu.VMEM)
    return pl.pallas_call(
        functools.partial(fused, half, cap),
        out_shape=jax.ShapeDtypeStruct((rows, width), bf),
        in_specs=[vmem] * 9,
        out_specs=vmem,
        scratch_shapes=[
            pltpu.VMEM((8, lanes), jnp.float32),
            pltpu.VMEM((8, lanes), jnp.float32),
            pltpu.VMEM((rows, width), bf),
            pltpu.VMEM((packed, width), bf),
            pltpu.VMEM((packed, width), bf),
            pltpu.VMEM((packed, width), bf),
            pltpu.VMEM((packed, width), bf),
            pltpu.VMEM((4, 2 * fpart, width), bf),
            pltpu.VMEM((hidden, width), bf),
            pltpu.VMEM((packed, hidden), bf),
            pltpu.VMEM((packed, hidden), bf),
            pltpu.VMEM((packed, width), bf),
            pltpu.VMEM((packed, width), bf),
            pltpu.VMEM((packed, width), bf),
            pltpu.VMEM((packed, width), bf),
            pltpu.VMEM((rows, width), bf),
            pltpu.VMEM((rows, width), bf),
            pltpu.VMEM((rows, width), jnp.float32),
            pltpu.SemaphoreType.DMA((copies,)),
            pltpu.SemaphoreType.DMA((copies,)),
        ],
        compiler_params=pltpu.CompilerParams(
            collective_id=0, has_side_effects=True, vmem_limit_bytes=56 * 1024 * 1024
        ),
    )(
        expert_ids.T,
        group_weight[None, :],
        expert_share.T,
        tokens,
        gate_w[0],
        up_w[0],
        down_w[0],
        out_gain[None, :],
        out_shift[None, :],
    )


def solution(mesh):
    paired = mesh.shape["tp"] == 4 and mesh.shape["ep"] % 2 == 0
    placed = (
        P(("ep", "tp"), None),
        P(("ep", "tp"), None),
        P(("ep", "tp")),
        P(("ep", "tp"), None),
        P("ep", "tp", None),
        P("ep", "tp", None),
        P("ep", "tp", None),
        P(),
        P(),
    )
    return jax.shard_map(
        fast_body if paired else body, mesh=mesh, in_specs=placed, out_specs=P(("ep", "tp"), None), check_vma=False
    )
```

```python
import functools

import jax
import jax.numpy as jnp
from jax import lax
from jax.experimental import pallas as pl
from jax.experimental.pallas import tpu as pltpu
from jax.sharding import PartitionSpec as P

TOP = 2


residual_scale = 2.0**0.5
norm_eps = 1e-05


def layer_norm(values, gain, shift):
    center = values - jnp.mean(values, axis=-1, keepdims=True)
    variance = jnp.mean(center * center, axis=-1, keepdims=True)
    return (center * lax.rsqrt(variance + norm_eps) * gain + shift).astype(jnp.bfloat16)


def body(tokens, expert_ids, group_weight, expert_share, gate_w, up_w, down_w, out_gain, out_shift):
    tok_count, model_width = tokens.shape
    ep_size = lax.axis_size("ep")
    local_count = gate_w.shape[0]
    experts_all = ep_size * local_count
    capacity = 3 * tok_count * TOP // (2 * experts_all)
    flat_ids = expert_ids.reshape(-1)
    onehot = (flat_ids[:, None] == jnp.arange(experts_all, dtype=jnp.int32)[None, :]).astype(
        jnp.int32
    )
    earlier = jnp.cumsum(onehot, axis=0) - onehot
    slot_index = jnp.sum(earlier * onehot, axis=1)
    dest_index = flat_ids * capacity + slot_index
    copies = jnp.repeat(tokens, TOP, axis=0)
    send_buf = (
        jnp.zeros((experts_all * capacity, model_width), tokens.dtype).at[dest_index].set(copies)
    )
    send_buf = send_buf.reshape(ep_size, local_count * capacity, model_width)
    received = lax.all_to_all(send_buf, "ep", split_axis=0, concat_axis=0, tiled=True)
    expert_rows = received.reshape(ep_size, local_count, capacity, model_width)
    expert_rows = expert_rows.transpose(1, 0, 2, 3).reshape(
        local_count, ep_size * capacity, model_width
    )
    gate_piece = lax.all_gather(gate_w, "tp", axis=1, tiled=True)
    up_piece = lax.all_gather(up_w, "tp", axis=1, tiled=True)
    down_piece = lax.all_gather(down_w, "tp", axis=1, tiled=True)
    gate_act = jnp.einsum(
        "lrd,lfd->lrf", expert_rows, gate_piece, preferred_element_type=jnp.float32
    )
    up_act = jnp.einsum("lrd,lfd->lrf", expert_rows, up_piece, preferred_element_type=jnp.float32)
    hidden = (jax.nn.silu(gate_act) * up_act).astype(jnp.bfloat16)
    expert_out = jnp.einsum("lrf,lfd->lrd", hidden, down_piece, preferred_element_type=jnp.float32)
    results = expert_out.astype(jnp.bfloat16).reshape(local_count, ep_size, capacity, model_width)
    results = results.transpose(1, 0, 2, 3).reshape(ep_size, local_count * capacity, model_width)
    returned = lax.all_to_all(results, "ep", split_axis=0, concat_axis=0, tiled=True)
    returned = returned.reshape(experts_all * capacity, model_width)
    picked = returned[dest_index].reshape(tok_count, TOP, model_width)
    share_norm = expert_share / jnp.sum(expert_share, axis=1, keepdims=True)
    route_weight = group_weight[:, None] * share_norm
    mixture = jnp.sum(route_weight[:, :, None] * picked.astype(jnp.float32), axis=1)
    residual = residual_scale * tokens.astype(jnp.float32) + mixture
    return layer_norm(residual, out_gain, out_shift)


MESH = pl.DeviceIdType.MESH
OUTWARD = (2, 2, 2, 1, 1)
INWARD = (1, 1, 2, 2, 2)


def cdot(a, b):
    return jnp.dot(a, b, preferred_element_type=jnp.float32)


def ndot(a, b, precision=None):
    return lax.dot_general(
        a, b, (((1,), (1,)), ((), ())), precision=precision, preferred_element_type=jnp.float32
    )


def fused(
    half, cap, ids_ref, group_ref, share_ref, tok_ref, gate_ref, up_ref, down_ref, gain_ref,
    shift_ref, out_ref, meta, mmeta, mtok, send_own, send_mir, recv_own, recv_mir, wgu, wd,
    hid_own, hid_mir, res_own, res_mir, ret_own, ret_mir, part, mpart, total, acts, send_sem, recv_sem,
    own_sem,
):
    rows, width = tok_ref.shape
    fpart = gate_ref.shape[0]
    unit = width // 8
    outward = [pl.ds(sum(OUTWARD[:c]) * unit, n * unit) for c, n in enumerate(OUTWARD)]
    inward = [pl.ds(sum(INWARD[:c]) * unit, n * unit) for c, n in enumerate(INWARD)]
    sides = [pl.ds(0, width // 2), pl.ds(width // 2, width // 2)]
    ep, tp = lax.axis_index("ep"), lax.axis_index("tp")
    lo = lax.rem(ep, half)
    base = ep - lo
    mirror = {"ep": lax.rem(ep + half, 2 * half)}
    pair = {"tp": tp + 1 - 2 * lax.rem(tp, 2)}
    across = {"tp": lax.rem(tp + 2, 4)}
    ahead = [{"ep": base + lax.rem(lo + r, half)} for r in range(half)]
    behind = [{"ep": base + lax.rem(lo + half - r, half)} for r in range(half)]

    barrier = pltpu.get_barrier_semaphore()
    peers = [mirror, pair, across] + ahead[1:]
    for peer in peers:
        pl.semaphore_signal(barrier, inc=1, device_id=peer, device_id_type=MESH)
    pl.semaphore_wait(barrier, len(peers))

    started = []

    def send(src, dst, peer):
        i = len(started)
        copy = pltpu.make_async_remote_copy(
            src_ref=src, dst_ref=dst, send_sem=send_sem.at[i], recv_sem=recv_sem.at[i],
            device_id=peer, device_id_type=MESH,
        )
        copy.start()
        started.append(copy)
        return copy

    def block(r):
        return pl.ds(r * cap, cap)

    meta[...] = jnp.zeros_like(meta)
    share = share_ref[...]
    weight = group_ref[...] * (share / jnp.sum(share, axis=0, keepdims=True))
    meta[0:2, 0:rows] = ids_ref[...].astype(jnp.float32)
    meta[2:4, 0:rows] = weight
    gate_rows, up_rows = pl.ds(0, fpart), pl.ds(fpart, fpart)
    tok_in = []

    def cross():
        at = outward[len(tok_in)]
        tok_in.append(send(tok_ref.at[:, at], mtok.at[:, at], mirror))

    def wrows(s):
        return pl.ds(s * fpart, fpart)

    cross()
    local = [
        pltpu.make_async_copy(src, dst, own_sem.at[i])
        for i, (src, dst) in enumerate(
            [
                (gate_ref, wgu.at[0, gate_rows]),
                (up_ref, wgu.at[0, up_rows]),
                (down_ref, wd.at[wrows(0)]),
            ]
        )
    ]
    for copy in local:
        copy.start()
    gate2 = send(gate_ref, wgu.at[2, gate_rows], across)
    up2 = send(up_ref, wgu.at[2, up_rows], across)
    down2 = [send(down_ref.at[:, side], wd.at[wrows(2), side], across) for side in sides]
    gate1 = send(gate_ref, wgu.at[1, gate_rows], pair)
    up1 = send(up_ref, wgu.at[1, up_rows], pair)
    down1 = send(down_ref, wd.at[wrows(1)], pair)
    meta_in = send(meta, mmeta, mirror)

    earlier = lax.broadcasted_iota(jnp.int32, (rows, rows), 0)
    later = lax.broadcasted_iota(jnp.int32, (rows, rows), 1)
    before = (earlier < later).astype(jnp.bfloat16)
    same = (earlier == later).astype(jnp.float32)
    names = (base + lax.rem(lo + lax.broadcasted_iota(jnp.int32, (8, rows), 0), half)).astype(
        jnp.float32
    )

    def routing(table):
        first, second = table[0:1, 0:rows] == names, table[1:2, 0:rows] == names
        hits = jnp.where(first | second, 1.0, 0.0)
        slots = cdot(hits.astype(jnp.bfloat16), before)
        key = jnp.where(hits > 0.5, slots, -1.0)
        value = jnp.where(first, table[2:3, 0:rows], 0.0) + jnp.where(
            second, table[3:4, 0:rows], 0.0
        )
        place = lax.broadcasted_iota(jnp.int32, (cap, rows), 0).astype(jnp.float32)
        pick = jnp.concatenate(
            [jnp.where(place == key[r : r + 1], 1.0, 0.0) for r in range(half)], axis=0
        ).astype(jnp.bfloat16)
        key_col = ndot(same, key, lax.Precision.HIGHEST)
        value_col = ndot(same, value, lax.Precision.HIGHEST)
        lane = lax.broadcasted_iota(jnp.int32, (rows, half * cap), 1)
        merge = jnp.zeros((rows, half * cap), jnp.float32)
        for r in range(half):
            at = (lane - r * cap).astype(jnp.float32) == key_col[:, r : r + 1]
            at = at & (lane >= r * cap)
            merge = jnp.where(at, value_col[:, r : r + 1], merge)
        high = merge.astype(jnp.bfloat16)
        low = (merge - high.astype(jnp.float32)).astype(jnp.bfloat16)
        return pick, high, low

    def pack(pick, source, send_buf, recv_buf, at):
        packed = cdot(pick, source[:, at]).astype(jnp.bfloat16)
        recv_buf[block(0), at] = packed[0:cap]
        send_buf[:, at] = packed

    def scatter(send_buf, recv_buf, at, peers):
        return [
            send(send_buf.at[block(r), at], recv_buf.at[block(r), at], peers[r])
            for r in range(1, half)
        ]

    def pack_mirrored():
        c = len(mir_in)
        tok_in[c].wait_recv()
        pack(pick_mir, mtok, send_mir, recv_mir, outward[c])
        mir_in.append(scatter(send_mir, recv_mir, outward[c], ahead))

    def arrived(copies):
        for copy in copies:
            copy.wait_recv()

    def activate(both):
        gate, up = both[:, 0:fpart], both[:, fpart : 2 * fpart]
        return (gate / (1.0 + jnp.exp(-gate)) * up).astype(jnp.bfloat16)

    def gate_up(s):
        hid_own[:, wrows(s)] = activate(ndot(recv_own[...], wgu[s]))

    pick_own, high_own, low_own = routing(meta)
    for side in sides:
        pack(pick_own, tok_ref, send_own, recv_own, side)
    cross()
    own_in = scatter(send_own, recv_own, pl.ds(0, width), ahead)
    cross()
    cross()
    cross()
    mir_in = []
    meta_in.wait_recv()
    pick_mir, high_mir, low_mir = routing(mmeta)
    pack_mirrored()
    gate2.wait_recv()
    gate3 = send(wgu.at[2, gate_rows], wgu.at[3, gate_rows], pair)
    pack_mirrored()
    arrived(own_in + [gate1, up1])
    for copy in local:
        copy.wait()
    gate_up(0)
    gate_up(1)
    pack_mirrored()
    up2.wait_recv()
    up3 = send(wgu.at[2, up_rows], wgu.at[3, up_rows], pair)
    gate_up(2)
    pack_mirrored()
    arrived([gate3, up3])
    gate_up(3)
    down2[0].wait_recv()
    down3 = [send(wd.at[wrows(2), sides[0]], wd.at[wrows(3), sides[0]], pair)]
    pack_mirrored()

    main = width - OUTWARD[-1] * unit
    for copies in mir_in[:-1]:
        arrived(copies)
    for s in range(4):
        acts[s] = ndot(recv_mir[:, 0:main], wgu[s, :, 0:main])

    def project(hid, res, ret, at):
        result = cdot(hid[...], wd[:, at]).astype(jnp.bfloat16)
        ret[block(0), at] = result[0:cap]
        res[:, at] = result
        return scatter(res, ret, at, behind)

    def combine(high, low, ret, at):
        return cdot(high, ret[:, at]) + cdot(low, ret[:, at])

    arrived([down1, down3[0]])
    arrived(mir_in[-1])
    for s in range(4):
        hid_mir[:, wrows(s)] = activate(
            acts[s] + ndot(recv_mir[:, main:width], wgu[s, :, main:width])
        )
    back_mir = [project(hid_mir, res_mir, ret_mir, inward[0])]
    back_mir.append(project(hid_mir, res_mir, ret_mir, inward[1]))
    part_in = []

    def give_back():
        c = len(part_in)
        at = inward[c]
        arrived(back_mir[c])
        part[:, at] = combine(high_mir, low_mir, ret_mir, at).astype(jnp.bfloat16)
        part_in.append(send(part.at[:, at], mpart.at[:, at], mirror))

    back_mir.append(project(hid_mir, res_mir, ret_mir, inward[2]))
    give_back()
    back_own = project(hid_own, res_own, ret_own, sides[0])
    give_back()
    down2[1].wait_recv()
    down3.append(send(wd.at[wrows(2), sides[1]], wd.at[wrows(3), sides[1]], pair))
    give_back()
    down3[1].wait_recv()
    back_mir.append(project(hid_mir, res_mir, ret_mir, inward[3]))
    back_mir.append(project(hid_mir, res_mir, ret_mir, inward[4]))
    back_own += project(hid_own, res_own, ret_own, sides[1])
    give_back()
    give_back()
    arrived(back_own)
    for at in inward:
        total[:, at] = residual_scale * tok_ref[:, at].astype(jnp.float32) + combine(
            high_own, low_own, ret_own, at
        )
    mean = jnp.zeros((rows, 1), jnp.float32)
    for copy, at in zip(part_in, inward):
        copy.wait_recv()
        piece = total[:, at] + mpart[:, at].astype(jnp.float32)
        total[:, at] = piece
        mean = mean + jnp.sum(piece, axis=1, keepdims=True)
    mean = mean / width
    center = total[...] - mean
    variance = jnp.sum(center * center, axis=1, keepdims=True) / width
    out_ref[...] = (
        center * lax.rsqrt(variance + norm_eps) * gain_ref[...] + shift_ref[...]
    ).astype(jnp.bfloat16)
    for copy in started:
        copy.wait_send()


def fast_body(
    tokens, expert_ids, group_weight, expert_share, gate_w, up_w, down_w, out_gain, out_shift
):
    rows, width = tokens.shape
    experts = lax.axis_size("ep")
    half = experts // 2
    fpart = gate_w.shape[1]
    hidden = fpart * lax.axis_size("tp")
    cap = -(-(3 * rows * TOP // (2 * experts)) // 16) * 16
    lanes = -(-rows // 128) * 128
    packed = half * cap
    parts = len(OUTWARD) + len(INWARD)
    copies = 12 + parts + (half - 1) * (parts + 3)
    bf = jnp.bfloat16
    vmem = pl.BlockSpec(memory_space=pltpu.VMEM)
    return pl.pallas_call(
        functools.partial(fused, half, cap),
        out_shape=jax.ShapeDtypeStruct((rows, width), bf),
        in_specs=[vmem] * 4 + [pl.BlockSpec(memory_space=pl.ANY)] * 3 + [vmem] * 2,
        out_specs=vmem,
        scratch_shapes=[
            pltpu.VMEM((8, lanes), jnp.float32),
            pltpu.VMEM((8, lanes), jnp.float32),
            pltpu.VMEM((rows, width), bf),
            pltpu.VMEM((packed, width), bf),
            pltpu.VMEM((packed, width), bf),
            pltpu.VMEM((packed, width), bf),
            pltpu.VMEM((packed, width), bf),
            pltpu.VMEM((4, 2 * fpart, width), bf),
            pltpu.VMEM((hidden, width), bf),
            pltpu.VMEM((packed, hidden), bf),
            pltpu.VMEM((packed, hidden), bf),
            pltpu.VMEM((packed, width), bf),
            pltpu.VMEM((packed, width), bf),
            pltpu.VMEM((packed, width), bf),
            pltpu.VMEM((packed, width), bf),
            pltpu.VMEM((rows, width), bf),
            pltpu.VMEM((rows, width), bf),
            pltpu.VMEM((rows, width), jnp.float32),
            pltpu.VMEM((4, packed, 2 * fpart), jnp.float32),
            pltpu.SemaphoreType.DMA((copies,)),
            pltpu.SemaphoreType.DMA((copies,)),
            pltpu.SemaphoreType.DMA((3,)),
        ],
        compiler_params=pltpu.CompilerParams(
            collective_id=0, has_side_effects=True, vmem_limit_bytes=56 * 1024 * 1024
        ),
    )(
        expert_ids.T,
        group_weight[None, :],
        expert_share.T,
        tokens,
        gate_w[0],
        up_w[0],
        down_w[0],
        out_gain[None, :],
        out_shift[None, :],
    )


def solution(mesh):
    paired = mesh.shape["tp"] == 4 and mesh.shape["ep"] % 2 == 0
    placed = (
        P(("ep", "tp"), None),
        P(("ep", "tp"), None),
        P(("ep", "tp")),
        P(("ep", "tp"), None),
        P("ep", "tp", None),
        P("ep", "tp", None),
        P("ep", "tp", None),
        P(),
        P(),
    )
    return jax.shard_map(
        fast_body if paired else body, mesh=mesh, in_specs=placed, out_specs=P(("ep", "tp"), None), check_vma=False
    )
```
